32 devices in a mesh: sp: 8 (over z, x), dp: 4 (over y, core).
Axes of the slice: x: 2, y: 2, z: 4, core: 2. Of those that a mesh axis runs over, the one named last changes fastest.
Arguments:
- inputs: bfloat16 [1536, 2048], P('sp'), may hold values from -6 to 6
- w_query: bfloat16 [2048, 2048], P('dp'), may hold values from -0.125 to 0.125
- w_key: bfloat16 [1024, 2048], P('dp'), may hold values from -0.125 to 0.125
- w_value: bfloat16 [1024, 2048], P('dp'), may hold values from -0.125 to 0.125
- query_gain: float32 [64], replicated, may hold values from 0.6 to 7
- key_gain: float32 [64], replicated, may hold values from 0.6 to 7
- grad_out: bfloat16 [1536, 2048], P('sp', 'dp'), may hold values from -6 to 6
Outputs:
- d_inputs: bfloat16 [1536, 2048], P('sp', 'dp')
- grad_wq: float32 [2048, 2048], P('dp')
- grad_wk: float32 [1024, 2048], P('dp')
- grad_wv: float32 [1024, 2048], P('dp')
The draws below stay inside these ranges and needn't reach their ends.
All inputs are finite; a program needn't handle non-finite values.
Results may differ from the reference program's by a relative error of at most 0.019.
The reference program's roundings to bfloat16 on the way count: a program that leaves them out, or rounds other values in their place, can miss the bound.
Values may be sent and summed in bfloat16 or wider, within the bound.
A program may use at most 64 MiB of HBM per device.

```python
import math
import jax
import jax.numpy as jnp
from jax import lax

D = 2048
HEAD_WIDTH = 64
QHEADS = 32
KEY_VALUE_HEADS = 16
GRID_W = 64
SEQUENCE_TOKENS = 1536
N_DP = 4


def gain_values(key):
    return jnp.exp(jax.random.uniform(key, (HEAD_WIDTH,), jnp.float32, math.log(0.6), math.log(1.6)))


def draw_query_gain(key, part):
    return gain_values(jax.random.fold_in(key, 31))


def draw_key_gain(key, part):
    return gain_values(jax.random.fold_in(key, 47))


def levels(key, shape, cuts, least, high):
    level = 1.0
    for position, blocks in cuts:
        draws = jax.random.uniform(jax.random.fold_in(jax.random.fold_in(key, 6), position), (blocks,), jnp.float32, least / len(cuts), high / len(cuts))
        level = level * jnp.repeat(jnp.exp(draws), shape[position] // blocks).reshape((-1,) + (1,) * (len(shape) - 1 - position))
    return level


def gaussian(stream_key, dims, scale, reach, split=(), kind=jnp.bfloat16):
    values = scale * jax.random.normal(stream_key, dims, jnp.float32)
    if split:
        values = values * levels(stream_key, dims, split, -0.22, 0.18)
    return jnp.clip(values, -reach, reach).astype(kind)


def setup_inputs(seed: int = 0) -> dict:
    arg_keys = jax.random.split(jax.random.key(seed), 8)
    return {
        "inputs": gaussian(arg_keys[0], (SEQUENCE_TOKENS, D), 1.0, 6.0, ((0, 8),)),
        "w_query": gaussian(arg_keys[1], (QHEADS * HEAD_WIDTH, D), D ** -0.5, 0.125, ((0, 4),)),
        "w_key": gaussian(arg_keys[2], (KEY_VALUE_HEADS * HEAD_WIDTH, D), D ** -0.5, 0.125, ((0, 4),)),
        "w_value": gaussian(arg_keys[3], (KEY_VALUE_HEADS * HEAD_WIDTH, D), D ** -0.5, 0.125, ((0, 4),)),
        "query_gain": draw_query_gain(jax.random.fold_in(arg_keys[7], 71), 0),
        "key_gain": draw_key_gain(jax.random.fold_in(arg_keys[7], 71), 0),
        "grad_out": gaussian(arg_keys[6], (SEQUENCE_TOKENS, QHEADS * HEAD_WIDTH), 1.0, 6.0, ((0, 8), (1, 4))),
    }


norm_eps = 1e-06
axial_base = 10000.0

def rotation_tables(offset, count):
    positions = offset + jnp.arange(count, dtype=jnp.int32)
    grid_rows = (positions // GRID_W).astype(jnp.float32)
    grid_cols = (positions % GRID_W).astype(jnp.float32)
    quarter = HEAD_WIDTH // 4
    freqs_axis = axial_base ** (-jnp.arange(quarter, dtype=jnp.float32) / quarter)
    angle_rows = grid_rows[:, None] * freqs_axis[None, :]
    angle_cols = grid_cols[:, None] * freqs_axis[None, :]
    cosine = jnp.concatenate([jnp.cos(angle_rows), jnp.cos(angle_rows), jnp.cos(angle_cols), jnp.cos(angle_cols)], axis=1)
    sine = jnp.concatenate([jnp.sin(angle_rows), jnp.sin(angle_rows), jnp.sin(angle_cols), jnp.sin(angle_cols)], axis=1)
    return (cosine, sine)

def quarter_turn(values):
    quarter = HEAD_WIDTH // 4
    return jnp.concatenate([-values[..., quarter:2 * quarter], values[..., :quarter], -values[..., 3 * quarter:], values[..., 2 * quarter:3 * quarter]], axis=-1)

def quarter_back(values):
    quarter = HEAD_WIDTH // 4
    return jnp.concatenate([values[..., quarter:2 * quarter], -values[..., :quarter], values[..., 3 * quarter:], -values[..., 2 * quarter:3 * quarter]], axis=-1)

def rotate(values, cosine, sine):
    return values * cosine + quarter_turn(values) * sine

def rotate_back(grads, cosine, sine):
    return grads * cosine + quarter_back(grads * sine)

def head_norm(raw):
    scale_inv = lax.rsqrt(lax.optimization_barrier(jnp.mean(raw * raw, axis=-1, keepdims=True)) + norm_eps)
    return (raw * scale_inv, scale_inv)

def head_norm_back(grads, normed, scale_inv, gain):
    scaled = grads * gain
    return scale_inv * (scaled - normed * lax.optimization_barrier(jnp.mean(scaled * normed, axis=-1, keepdims=True)))

def reference(inputs, w_query, w_key, w_value, query_gain, key_gain, grad_out):
    group = QHEADS // KEY_VALUE_HEADS
    scale = HEAD_WIDTH ** (-0.5)
    cosine, sine = rotation_tables(0, SEQUENCE_TOKENS)
    cos_wide = cosine[:, None, :]
    sin_wide = sine[:, None, :]
    q_raw = jnp.dot(inputs, w_query.T, preferred_element_type=jnp.float32).astype(jnp.bfloat16)
    k_raw = jnp.dot(inputs, w_key.T, preferred_element_type=jnp.float32).astype(jnp.bfloat16)
    v_raw = jnp.dot(inputs, w_value.T, preferred_element_type=jnp.float32).astype(jnp.bfloat16)
    q_wide = lax.optimization_barrier(q_raw).astype(jnp.float32).reshape(SEQUENCE_TOKENS, QHEADS, HEAD_WIDTH)
    k_wide = lax.optimization_barrier(k_raw).astype(jnp.float32).reshape(SEQUENCE_TOKENS, KEY_VALUE_HEADS, HEAD_WIDTH)
    q_normed, q_inv = head_norm(q_wide)
    k_normed, k_inv = head_norm(k_wide)
    q_rot = rotate(q_normed * query_gain, cos_wide, sin_wide).astype(jnp.bfloat16)
    k_rot = rotate(k_normed * key_gain, cos_wide, sin_wide).astype(jnp.bfloat16)
    query_heads = q_rot.reshape(SEQUENCE_TOKENS, KEY_VALUE_HEADS, group, HEAD_WIDTH).transpose(1, 0, 2, 3)
    gradient_heads = grad_out.reshape(SEQUENCE_TOKENS, KEY_VALUE_HEADS, group, HEAD_WIDTH).transpose(1, 0, 2, 3)
    key_heads = k_rot.transpose(1, 0, 2)
    value_heads = v_raw.reshape(SEQUENCE_TOKENS, KEY_VALUE_HEADS, HEAD_WIDTH).transpose(1, 0, 2)

    def single_key_head(operands):
        query_rot, key_rot, value_rows, grad_rows = operands
        grad_query = []
        grad_key = jnp.zeros((SEQUENCE_TOKENS, HEAD_WIDTH), jnp.float32)
        grad_value = jnp.zeros((SEQUENCE_TOKENS, HEAD_WIDTH), jnp.float32)
        for member in range(group):
            query_head = query_rot[:, member]
            grad_head = grad_rows[:, member]
            scores = jnp.dot(query_head, key_rot.T, preferred_element_type=jnp.float32) * scale
            maxima = lax.optimization_barrier(jnp.max(scores, axis=1, keepdims=True))
            log_total = maxima + jnp.log(lax.optimization_barrier(jnp.sum(jnp.exp(scores - maxima), axis=1, keepdims=True)))
            prob_exact = jnp.exp(scores - log_total)
            prob_half = prob_exact.astype(jnp.bfloat16)
            attn_rows = jnp.dot(prob_half, value_rows, preferred_element_type=jnp.float32).astype(jnp.bfloat16)
            attn_wide = lax.optimization_barrier(attn_rows).astype(jnp.float32)
            delta_rows = lax.optimization_barrier(jnp.sum(grad_head.astype(jnp.float32) * attn_wide, axis=1, keepdims=True))
            grad_value = grad_value + jnp.dot(prob_half.T, grad_head, preferred_element_type=jnp.float32)
            dprob = jnp.dot(grad_head, value_rows.T, preferred_element_type=jnp.float32)
            dscore = (prob_exact * (dprob - delta_rows)).astype(jnp.bfloat16)
            grad_query.append(jnp.dot(dscore, key_rot, preferred_element_type=jnp.float32) * scale)
            grad_key = grad_key + jnp.dot(dscore.T, query_head, preferred_element_type=jnp.float32) * scale
        return (jnp.stack(grad_query, axis=1), grad_key, grad_value)
    gradient_query_rotated, gradient_key_rotated, gradient_value_rotated = lax.map(single_key_head, (query_heads, key_heads, value_heads, gradient_heads))
    gradient_query_rotated = gradient_query_rotated.transpose(1, 0, 2, 3).reshape(SEQUENCE_TOKENS, QHEADS, HEAD_WIDTH)
    gradient_key_rotated = gradient_key_rotated.transpose(1, 0, 2)
    gradient_values = gradient_value_rotated.transpose(1, 0, 2).reshape(SEQUENCE_TOKENS, KEY_VALUE_HEADS * HEAD_WIDTH).astype(jnp.bfloat16)
    grad_q = head_norm_back(rotate_back(gradient_query_rotated, cos_wide, sin_wide), q_normed, q_inv, query_gain)
    grad_q = grad_q.reshape(SEQUENCE_TOKENS, QHEADS * HEAD_WIDTH).astype(jnp.bfloat16)
    grad_k = head_norm_back(rotate_back(gradient_key_rotated, cos_wide, sin_wide), k_normed, k_inv, key_gain)
    grad_k = grad_k.reshape(SEQUENCE_TOKENS, KEY_VALUE_HEADS * HEAD_WIDTH).astype(jnp.bfloat16)
    query_cols = QHEADS * HEAD_WIDTH // N_DP
    key_cols = KEY_VALUE_HEADS * HEAD_WIDTH // N_DP
    total = jnp.zeros((SEQUENCE_TOKENS, D), jnp.float32)
    for group_index in range(N_DP):
        q_lo = group_index * query_cols
        k_lo = group_index * key_cols
        head_part = jnp.dot(grad_q[:, q_lo:q_lo + query_cols], w_query[q_lo:q_lo + query_cols], preferred_element_type=jnp.float32)
        head_part = head_part + jnp.dot(grad_k[:, k_lo:k_lo + key_cols], w_key[k_lo:k_lo + key_cols], preferred_element_type=jnp.float32)
        head_part = head_part + jnp.dot(gradient_values[:, k_lo:k_lo + key_cols], w_value[k_lo:k_lo + key_cols], preferred_element_type=jnp.float32)
        rounded = lax.optimization_barrier(head_part.astype(jnp.bfloat16))
        total = total + rounded.astype(jnp.float32)
    d_inputs = total.astype(jnp.bfloat16)
    grad_wq = jnp.dot(grad_q.T, inputs, preferred_element_type=jnp.float32)
    grad_wk = jnp.dot(grad_k.T, inputs, preferred_element_type=jnp.float32)
    grad_wv = jnp.dot(gradient_values.T, inputs, preferred_element_type=jnp.float32)
    return (d_inputs, grad_wq, grad_wk, grad_wv)
```

```python
import functools

import jax
import jax.numpy as jnp
from jax import lax
from jax.experimental import pallas as pl
from jax.experimental.pallas import tpu as pltpu
from jax.sharding import PartitionSpec as P

HEAD_WIDTH = 64
GRID_W = 64


norm_eps = 1e-06
axial_base = 10000.0


def rotation_tables(offset, count):
    positions = offset + jnp.arange(count, dtype=jnp.int32)
    grid_rows = (positions // GRID_W).astype(jnp.float32)
    grid_cols = (positions % GRID_W).astype(jnp.float32)
    quarter = HEAD_WIDTH // 4
    freqs_axis = axial_base ** (-jnp.arange(quarter, dtype=jnp.float32) / quarter)
    angle_rows = grid_rows[:, None] * freqs_axis[None, :]
    angle_cols = grid_cols[:, None] * freqs_axis[None, :]
    cosine = jnp.concatenate(
        [jnp.cos(angle_rows), jnp.cos(angle_rows), jnp.cos(angle_cols), jnp.cos(angle_cols)], axis=1
    )
    sine = jnp.concatenate(
        [jnp.sin(angle_rows), jnp.sin(angle_rows), jnp.sin(angle_cols), jnp.sin(angle_cols)], axis=1
    )
    return (cosine, sine)


def quarter_turn(values):
    quarter = HEAD_WIDTH // 4
    return jnp.concatenate(
        [
            -values[..., quarter : 2 * quarter],
            values[..., :quarter],
            -values[..., 3 * quarter :],
            values[..., 2 * quarter : 3 * quarter],
        ],
        axis=-1,
    )


def quarter_back(values):
    quarter = HEAD_WIDTH // 4
    return jnp.concatenate(
        [
            values[..., quarter : 2 * quarter],
            -values[..., :quarter],
            values[..., 3 * quarter :],
            -values[..., 2 * quarter : 3 * quarter],
        ],
        axis=-1,
    )


def rotate(values, cosine, sine):
    return values * cosine + quarter_turn(values) * sine


def rotate_back(grads, cosine, sine):
    return grads * cosine + quarter_back(grads * sine)


def head_norm(raw):
    scale_inv = lax.rsqrt(jnp.mean(raw * raw, axis=-1, keepdims=True) + norm_eps)
    return (raw * scale_inv, scale_inv)


def head_norm_back(grads, normed, scale_inv, gain):
    scaled = grads * gain
    return scale_inv * (scaled - normed * jnp.mean(scaled * normed, axis=-1, keepdims=True))


def body(inputs, w_query, w_key, w_value, query_gain, key_gain, grad_out):
    tok_rows = inputs.shape[0]
    local_query = w_query.shape[0] // HEAD_WIDTH
    local_keys = w_key.shape[0] // HEAD_WIDTH
    group = local_query // local_keys
    key_width = local_keys * HEAD_WIDTH
    scale = HEAD_WIDTH ** (-0.5)
    contract = (((1,), (1,)), ((), ()))
    leading = (((0,), (0,)), ((), ()))
    offset = lax.axis_index("sp") * tok_rows
    cosine, sine = rotation_tables(offset, tok_rows)
    cos_wide = cosine[:, None, :]
    sin_wide = sine[:, None, :]
    q_raw = lax.dot_general(inputs, w_query, contract, preferred_element_type=jnp.float32).astype(
        jnp.bfloat16
    )
    w_pair = jnp.concatenate([w_key, w_value], axis=0)
    kv_raw = lax.dot_general(inputs, w_pair, contract, preferred_element_type=jnp.float32).astype(
        jnp.bfloat16
    )
    q_wide = (
        lax.optimization_barrier(q_raw)
        .astype(jnp.float32)
        .reshape(tok_rows, local_query, HEAD_WIDTH)
    )
    k_wide = (
        lax.optimization_barrier(kv_raw[:, :key_width])
        .astype(jnp.float32)
        .reshape(tok_rows, local_keys, HEAD_WIDTH)
    )
    q_normed, q_inv = head_norm(q_wide)
    k_normed, k_inv = head_norm(k_wide)
    q_rot = rotate(q_normed * query_gain, cos_wide, sin_wide).astype(jnp.bfloat16)
    k_rot = rotate(k_normed * key_gain, cos_wide, sin_wide).astype(jnp.bfloat16)
    kv_rot = jnp.concatenate([k_rot.reshape(tok_rows, key_width), kv_raw[:, key_width:]], axis=1)
    kv_every = lax.all_gather(kv_rot, "sp", axis=0, tiled=True)
    seq_rows = kv_every.shape[0]
    keys_every = kv_every[:, :key_width]
    values_every = kv_every[:, key_width:]
    grad_query = []
    log_totals = []
    deltas = []
    key_terms = [jnp.zeros((seq_rows, HEAD_WIDTH), jnp.float32) for slot in range(local_keys)]
    value_terms = [jnp.zeros((seq_rows, HEAD_WIDTH), jnp.float32) for slot in range(local_keys)]
    for member in range(local_query):
        kv_index = member // group
        query_head = q_rot[:, member, :]
        key_head = keys_every[:, kv_index * HEAD_WIDTH : (kv_index + 1) * HEAD_WIDTH]
        value_head = values_every[:, kv_index * HEAD_WIDTH : (kv_index + 1) * HEAD_WIDTH]
        grad_head = grad_out[:, member * HEAD_WIDTH : (member + 1) * HEAD_WIDTH]
        scores = (
            lax.dot_general(query_head, key_head, contract, preferred_element_type=jnp.float32)
            * scale
        )
        maxima = jnp.max(scores, axis=1, keepdims=True)
        log_total = maxima + jnp.log(jnp.sum(jnp.exp(scores - maxima), axis=1, keepdims=True))
        prob_exact = jnp.exp(scores - log_total)
        prob_half = prob_exact.astype(jnp.bfloat16)
        attn_rows = jnp.dot(prob_half, value_head, preferred_element_type=jnp.float32).astype(
            jnp.bfloat16
        )
        attn_wide = lax.optimization_barrier(attn_rows).astype(jnp.float32)
        delta_rows = jnp.sum(grad_head.astype(jnp.float32) * attn_wide, axis=1, keepdims=True)
        dprob = lax.dot_general(grad_head, value_head, contract, preferred_element_type=jnp.float32)
        dscore = (prob_exact * (dprob - delta_rows)).astype(jnp.bfloat16)
        grad_query.append(jnp.dot(dscore, key_head, preferred_element_type=jnp.float32) * scale)
        log_totals.append(log_total)
        deltas.append(delta_rows)
        value_terms[kv_index] = value_terms[kv_index] + lax.dot_general(
            prob_half, grad_head, leading, preferred_element_type=jnp.float32
        )
        key_terms[kv_index] = (
            key_terms[kv_index]
            + lax.dot_general(dscore, query_head, leading, preferred_element_type=jnp.float32)
            * scale
        )
    gradient_query_rotated = jnp.stack(grad_query, axis=1)
    partial_sums = jnp.concatenate(key_terms + value_terms, axis=1)
    own_grads = lax.psum_scatter(partial_sums, "sp", scatter_dimension=0, tiled=True)
    gradient_key_rotated = own_grads[:, :key_width].reshape(tok_rows, local_keys, HEAD_WIDTH)
    grad_q = head_norm_back(
        rotate_back(gradient_query_rotated, cos_wide, sin_wide), q_normed, q_inv, query_gain
    )
    grad_q = grad_q.reshape(tok_rows, local_query * HEAD_WIDTH).astype(jnp.bfloat16)
    grad_k = head_norm_back(
        rotate_back(gradient_key_rotated, cos_wide, sin_wide), k_normed, k_inv, key_gain
    )
    grad_kv = jnp.concatenate(
        [
            grad_k.reshape(tok_rows, key_width).astype(jnp.bfloat16),
            own_grads[:, key_width:].astype(jnp.bfloat16),
        ],
        axis=1,
    )
    head_part = jnp.dot(grad_q, w_query, preferred_element_type=jnp.float32)
    head_part = head_part + jnp.dot(grad_kv, w_pair, preferred_element_type=jnp.float32)
    d_inputs = lax.psum_scatter(
        head_part.astype(jnp.bfloat16), "dp", scatter_dimension=1, tiled=True
    )
    grad_wq = lax.dot_general(grad_q, inputs, leading, preferred_element_type=jnp.float32)
    grad_wkv = lax.dot_general(grad_kv, inputs, leading, preferred_element_type=jnp.float32)
    grad_wq, grad_wkv = lax.psum((grad_wq, grad_wkv), "sp")
    return (d_inputs, grad_wq, grad_wkv[:key_width], grad_wkv[key_width:])


MESH = pl.DeviceIdType.MESH
VMEM_LIMIT = 60 * 1024 * 1024


def turn(values):
    quarter = HEAD_WIDTH // 4
    return jnp.concatenate(
        [
            -values[quarter : 2 * quarter],
            values[:quarter],
            -values[3 * quarter :],
            values[2 * quarter : 3 * quarter],
        ],
        axis=0,
    )


def turn_back(values):
    return -turn(values)


def norm_cols(raw):
    inv = lax.rsqrt(jnp.mean(raw * raw, axis=0, keepdims=True) + norm_eps)
    return raw * inv, inv


def norm_cols_back(grads, normed, inv, gain):
    scaled = grads * gain
    return inv * (scaled - normed * jnp.mean(scaled * normed, axis=0, keepdims=True))


def other_of_pair(index):
    return index + 1 - 2 * lax.rem(index, 2)


def gather_kernel(n, x_ref, g_ref, xall, gall, xsend, xrecv, gsend, grecv, fsend, frecv, own):
    me = lax.axis_index("sp")
    core = lax.rem(lax.axis_index("dp"), 2)
    twin = other_of_pair(lax.axis_index("dp"))
    half = x_ref.shape[0] // 2
    mine = pl.ds(pl.multiple_of(core * half, 16), half)
    theirs = pl.ds(pl.multiple_of((1 - core) * half, 16), half)
    barrier = pltpu.get_barrier_semaphore()
    for off in range(1, n):
        pl.semaphore_signal(
            barrier, inc=1, device_id={"sp": lax.rem(me + off, n)}, device_id_type=MESH
        )
    pl.semaphore_signal(barrier, inc=1, device_id={"dp": twin}, device_id_type=MESH)
    pl.semaphore_wait(barrier, n)
    sends = []
    for off in range(1, n):
        peer = lax.rem(me + off, n)
        sends.append(
            pltpu.make_async_remote_copy(
                src_ref=g_ref.at[peer],
                dst_ref=gall.at[me],
                send_sem=gsend.at[off - 1],
                recv_sem=grecv.at[off - 1],
                device_id={"sp": peer},
                device_id_type=MESH,
            )
        )
        sends.append(
            pltpu.make_async_remote_copy(
                src_ref=x_ref.at[mine],
                dst_ref=xall.at[me, mine],
                send_sem=xsend.at[off - 1],
                recv_sem=xrecv.at[off - 1],
                device_id={"sp": peer},
                device_id_type=MESH,
            )
        )
    for copy in sends:
        copy.start()
    own_x = pltpu.make_async_copy(x_ref, xall.at[me], own.at[0])
    own_g = pltpu.make_async_copy(g_ref.at[me], gall.at[me], own.at[1])
    own_x.start()
    own_g.start()
    for off in range(1, n):
        source = lax.rem(me + n - off, n)
        pltpu.make_async_remote_copy(
            src_ref=xall.at[source, mine],
            dst_ref=xall.at[source, mine],
            send_sem=xsend.at[off - 1],
            recv_sem=xrecv.at[off - 1],
            device_id={"sp": source},
            device_id_type=MESH,
        ).wait_recv()
        pltpu.make_async_remote_copy(
            src_ref=xall.at[source, mine],
            dst_ref=xall.at[source, mine],
            send_sem=fsend.at[off - 1],
            recv_sem=frecv.at[off - 1],
            device_id={"dp": twin},
            device_id_type=MESH,
        ).start()
    for off in range(1, n):
        source = lax.rem(me + n - off, n)
        pltpu.make_async_remote_copy(
            src_ref=g_ref.at[source],
            dst_ref=gall.at[source],
            send_sem=gsend.at[off - 1],
            recv_sem=grecv.at[off - 1],
            device_id={"sp": source},
            device_id_type=MESH,
        ).wait_recv()
        forward = pltpu.make_async_remote_copy(
            src_ref=xall.at[source, mine],
            dst_ref=xall.at[source, theirs],
            send_sem=fsend.at[off - 1],
            recv_sem=frecv.at[off - 1],
            device_id={"dp": twin},
            device_id_type=MESH,
        )
        forward.wait()
    for copy in sends:
        copy.wait_send()
    own_x.wait()
    own_g.wait()


def gather_call(n, x, g_parts):
    rows, width = x.shape
    dma = pltpu.SemaphoreType.DMA
    return pl.pallas_call(
        functools.partial(gather_kernel, n),
        out_shape=(
            jax.ShapeDtypeStruct((n, rows, width), x.dtype),
            jax.ShapeDtypeStruct(g_parts.shape, g_parts.dtype),
        ),
        in_specs=[pl.BlockSpec(memory_space=pltpu.VMEM)] * 2,
        out_specs=[pl.BlockSpec(memory_space=pl.ANY)] * 2,
        scratch_shapes=[dma((n - 1,))] * 6 + [dma((2,))],
        compiler_params=pltpu.CompilerParams(
            collective_id=0, has_side_effects=True, vmem_limit_bytes=VMEM_LIMIT
        ),
        name="gather_tokens",
    )(x, g_parts)


def head_kernel(
    tile, x_ref, w_ref, g_ref, cos_ref, sin_ref, qg_ref, kg_ref,
    gq_ref, mine_ref, theirs_ref, kn_ref, rk_ref,
    q_t, q_n, q_r, k_t, v_t, k_s, v_s, g_t, k_n, k_r, dk, dv,
):
    seq = x_ref.shape[0]
    width = HEAD_WIDTH
    scale = width ** (-0.5)
    contract = (((1,), (1,)), ((), ()))

    @pl.loop(0, seq // tile)
    def _(step):
        cols = pl.ds(pl.multiple_of(step * tile, tile), tile)
        raw = lax.dot_general(
            w_ref[...], x_ref[cols, :], contract, preferred_element_type=jnp.float32
        ).astype(jnp.bfloat16)
        wide = raw.astype(jnp.float32)
        cosine = cos_ref[:, cols]
        sine = sin_ref[:, cols]
        normed, inv = norm_cols(wide[:width])
        gained = normed * qg_ref[...]
        rot = (gained * cosine + turn(gained) * sine).astype(jnp.bfloat16)
        q_t[:, cols] = (rot.astype(jnp.float32) * scale).astype(jnp.bfloat16)
        q_n[:, cols] = normed
        q_r[:, cols] = inv
        normed, inv = norm_cols(wide[width : 2 * width])
        gained = normed * kg_ref[...]
        rot = (gained * cosine + turn(gained) * sine).astype(jnp.bfloat16)
        k_t[:, cols] = rot
        k_s[cols, :] = rot.astype(jnp.float32).T.astype(jnp.bfloat16)
        k_n[:, cols] = normed
        k_r[:, cols] = inv
        v_t[:, cols] = raw[2 * width :]
        v_s[cols, :] = wide[2 * width :].T.astype(jnp.bfloat16)
        g_t[:, cols] = g_ref[cols, :].astype(jnp.float32).T.astype(jnp.bfloat16)

    dk[...] = jnp.zeros_like(dk)
    dv[...] = jnp.zeros_like(dv)

    @pl.loop(0, seq // tile)
    def _(step):
        cols = pl.ds(pl.multiple_of(step * tile, tile), tile)
        query = q_t[:, cols]
        grad = g_t[:, cols]
        scores = jnp.dot(k_s[...], query, preferred_element_type=jnp.float32)
        maxima = jnp.max(scores, axis=0, keepdims=True)
        powers = jnp.exp(scores - maxima)
        prob = powers * (1.0 / jnp.sum(powers, axis=0, keepdims=True))
        prob_half = prob.astype(jnp.bfloat16)
        attn = jnp.dot(v_t[...], prob_half, preferred_element_type=jnp.float32).astype(jnp.bfloat16)
        delta = jnp.sum(grad.astype(jnp.float32) * attn.astype(jnp.float32), axis=0, keepdims=True)
        dv[...] += lax.dot_general(grad, prob_half, contract, preferred_element_type=jnp.float32)
        dprob = jnp.dot(v_s[...], grad, preferred_element_type=jnp.float32)
        dscore = (prob * (dprob - delta)).astype(jnp.bfloat16)
        dk[...] += lax.dot_general(query, dscore, contract, preferred_element_type=jnp.float32)
        dq = jnp.dot(k_t[...], dscore, preferred_element_type=jnp.float32) * scale
        back = dq * cos_ref[:, cols] + turn_back(dq * sin_ref[:, cols])
        gq_ref[:, cols] = norm_cols_back(back, q_n[:, cols], q_r[:, cols], qg_ref[...]).astype(
            jnp.bfloat16
        )

    parity = lax.rem(lax.axis_index("sp"), 2)
    half = seq // 2
    own = pl.ds(pl.multiple_of(parity * half, 128), half)
    other = pl.ds(pl.multiple_of((1 - parity) * half, 128), half)
    mine_ref[0] = dk[:, own]
    mine_ref[1] = dv[:, own]
    theirs_ref[0] = dk[:, other].astype(jnp.bfloat16)
    theirs_ref[1] = dv[:, other].astype(jnp.bfloat16)
    kn_ref[...] = k_n[:, own]
    rk_ref[...] = k_r[:, own]


def head_call(x_all, w_head, g_head, cosine, sine, q_gain, k_gain):
    seq = x_all.shape[0]
    width = HEAD_WIDTH
    half = seq // 2
    f32, bf16 = jnp.float32, jnp.bfloat16
    tile = 256
    return pl.pallas_call(
        functools.partial(head_kernel, tile),
        out_shape=(
            jax.ShapeDtypeStruct((width, seq), bf16),
            jax.ShapeDtypeStruct((2, width, half), f32),
            jax.ShapeDtypeStruct((2, width, half), bf16),
            jax.ShapeDtypeStruct((width, half), f32),
            jax.ShapeDtypeStruct((1, half), f32),
        ),
        in_specs=[pl.BlockSpec(memory_space=pltpu.VMEM)] * 7,
        out_specs=[pl.BlockSpec(memory_space=pltpu.VMEM)] * 5,
        scratch_shapes=[
            pltpu.VMEM((width, seq), bf16),
            pltpu.VMEM((width, seq), f32),
            pltpu.VMEM((1, seq), f32),
            pltpu.VMEM((width, seq), bf16),
            pltpu.VMEM((width, seq), bf16),
            pltpu.VMEM((seq, width), bf16),
            pltpu.VMEM((seq, width), bf16),
            pltpu.VMEM((width, seq), bf16),
            pltpu.VMEM((width, seq), f32),
            pltpu.VMEM((1, seq), f32),
            pltpu.VMEM((width, seq), f32),
            pltpu.VMEM((width, seq), f32),
        ],
        compiler_params=pltpu.CompilerParams(vmem_limit_bytes=VMEM_LIMIT),
        name="one_head",
    )(x_all, w_head, g_head, cosine, sine, q_gain, k_gain)


def spread_kernel(
    n, gq_ref, mine_ref, theirs_ref, kn_ref, rk_ref, cos_ref, sin_ref, kg_ref,
    gq_all, gkv_all, landed, gkv, qsend, qrecv, ksend, krecv, own,
):
    me = lax.axis_index("sp")
    mate = other_of_pair(me)
    half = mine_ref.shape[2]

    def place(index):
        columns = pl.ds(pl.multiple_of(lax.rem(index, 2) * half, 128), half)
        return gkv_all.at[:, index // 2, :, columns]

    barrier = pltpu.get_barrier_semaphore()
    for off in range(1, n):
        pl.semaphore_signal(
            barrier, inc=1, device_id={"sp": lax.rem(me + off, n)}, device_id_type=MESH
        )
    pl.semaphore_wait(barrier, n - 1)
    swap = pltpu.make_async_remote_copy(
        src_ref=theirs_ref,
        dst_ref=landed,
        send_sem=own.at[0],
        recv_sem=own.at[1],
        device_id={"sp": mate},
        device_id_type=MESH,
    )
    swap.start()

    def copy_q(off):
        return pltpu.make_async_remote_copy(
            src_ref=gq_ref,
            dst_ref=gq_all.at[me],
            send_sem=qsend.at[off - 1],
            recv_sem=qrecv.at[off - 1],
            device_id={"sp": lax.rem(me + off, n)},
            device_id_type=MESH,
        )

    def copy_k(off):
        return pltpu.make_async_remote_copy(
            src_ref=gkv,
            dst_ref=place(me),
            send_sem=ksend.at[off - 1],
            recv_sem=krecv.at[off - 1],
            device_id={"sp": lax.rem(me + off, n)},
            device_id_type=MESH,
        )

    for off in range(1, n):
        copy_q(off).start()
    own_q = pltpu.make_async_copy(gq_ref, gq_all.at[me], own.at[2])
    own_q.start()
    swap.wait()
    dkey = mine_ref[0] + landed[0].astype(jnp.float32)
    back = dkey * cos_ref[...] + turn_back(dkey * sin_ref[...])
    gkv[0] = norm_cols_back(back, kn_ref[...], rk_ref[...], kg_ref[...]).astype(jnp.bfloat16)
    gkv[1] = (mine_ref[1] + landed[1].astype(jnp.float32)).astype(jnp.bfloat16)
    for off in range(1, n):
        copy_k(off).start()
    own_k = pltpu.make_async_copy(gkv, place(me), own.at[3])
    own_k.start()
    for off in range(1, n):
        source = lax.rem(me + n - off, n)
        copy_q(off).wait_send()
        copy_k(off).wait_send()
        pltpu.make_async_remote_copy(
            src_ref=gq_ref,
            dst_ref=gq_all.at[source],
            send_sem=qsend.at[off - 1],
            recv_sem=qrecv.at[off - 1],
            device_id={"sp": source},
            device_id_type=MESH,
        ).wait_recv()
        pltpu.make_async_remote_copy(
            src_ref=gkv,
            dst_ref=place(source),
            send_sem=ksend.at[off - 1],
            recv_sem=krecv.at[off - 1],
            device_id={"sp": source},
            device_id_type=MESH,
        ).wait_recv()
    own_q.wait()
    own_k.wait()


def spread_call(n, gq, mine, theirs, k_normed, k_inv, cosine, sine, k_gain):
    width, seq = gq.shape
    half = seq // 2
    bf16 = jnp.bfloat16
    dma = pltpu.SemaphoreType.DMA
    return pl.pallas_call(
        functools.partial(spread_kernel, n),
        out_shape=(
            jax.ShapeDtypeStruct((n, width, seq), bf16),
            jax.ShapeDtypeStruct((2, n // 2, width, seq), bf16),
        ),
        in_specs=[pl.BlockSpec(memory_space=pltpu.VMEM)] * 8,
        out_specs=[pl.BlockSpec(memory_space=pl.ANY)] * 2,
        scratch_shapes=[
            pltpu.VMEM((2, width, half), bf16),
            pltpu.VMEM((2, width, half), bf16),
            dma((n - 1,)),
            dma((n - 1,)),
            dma((n - 1,)),
            dma((n - 1,)),
            dma((4,)),
        ],
        compiler_params=pltpu.CompilerParams(
            collective_id=1, has_side_effects=True, vmem_limit_bytes=VMEM_LIMIT
        ),
        name="spread_grads",
    )(gq, mine, theirs, k_normed, k_inv, cosine, sine, k_gain)


def axial_columns(seq):
    quarter = HEAD_WIDTH // 4
    freqs = axial_base ** (-jnp.arange(quarter, dtype=jnp.float32) / quarter)
    grid_rows = -(-seq // GRID_W)
    by_row = freqs[:, None] * jnp.arange(grid_rows, dtype=jnp.float32)[None, :]
    by_col = freqs[:, None] * jnp.arange(GRID_W, dtype=jnp.float32)[None, :]

    def table(function):
        rows = jnp.repeat(function(by_row), GRID_W, axis=1)[:, :seq]
        cols = jnp.tile(function(by_col), (1, grid_rows))[:, :seq]
        return jnp.concatenate([rows, rows, cols, cols], axis=0)

    return table(jnp.cos), table(jnp.sin)


def head_body(n, inputs, w_query, w_key, w_value, query_gain, key_gain, grad_out):
    rows = inputs.shape[0]
    seq = rows * n
    width = HEAD_WIDTH
    me = lax.axis_index("sp")
    g_parts = grad_out.reshape(rows, n, width).transpose(1, 0, 2)
    cosine, sine = axial_columns(seq)
    w_head = jnp.concatenate(
        [
            lax.dynamic_slice_in_dim(w_query, me * width, width, 0),
            lax.dynamic_slice_in_dim(w_key, (me // 2) * width, width, 0),
            lax.dynamic_slice_in_dim(w_value, (me // 2) * width, width, 0),
        ],
        axis=0,
    )
    q_gain = query_gain[:, None]
    k_gain = key_gain[:, None]
    x_all, g_all = gather_call(n, inputs, g_parts)
    x_all = x_all.reshape(seq, inputs.shape[1])
    gq, mine, theirs, k_normed, k_inv = head_call(
        x_all, w_head, g_all.reshape(seq, width), cosine, sine, q_gain, k_gain
    )
    half = seq // 2
    start = (me % 2) * half
    gq_all, gkv_all = spread_call(
        n, gq, mine, theirs, k_normed, k_inv,
        lax.dynamic_slice_in_dim(cosine, start, half, 1),
        lax.dynamic_slice_in_dim(sine, start, half, 1),
        k_gain,
    )
    grads = [
        gq_all.reshape(n * width, seq),
        gkv_all[0].reshape(n // 2 * width, seq),
        gkv_all[1].reshape(n // 2 * width, seq),
    ]
    head_part = 0.0
    for grad, weight in zip(grads, (w_query, w_key, w_value)):
        own = lax.dynamic_slice_in_dim(grad, me * rows, rows, 1)
        head_part = head_part + lax.dot_general(
            own, weight, (((0,), (0,)), ((), ())), preferred_element_type=jnp.float32
        )
    d_inputs = lax.psum_scatter(
        head_part.astype(jnp.bfloat16), "dp", scatter_dimension=1, tiled=True
    )
    outs = [jnp.dot(grad, x_all, preferred_element_type=jnp.float32) for grad in grads]
    return (d_inputs, *outs)


def solution(mesh):
    n_sp = mesh.shape["sp"]
    n_dp = mesh.shape["dp"]

    def whole_body(inputs, w_query, w_key, *rest):
        heads = w_query.shape[0] // HEAD_WIDTH
        rows = inputs.shape[0]
        fits = heads == n_sp and w_query.shape[0] == 2 * w_key.shape[0] and n_dp % 2 == 0
        if fits and n_sp % 2 == 0 and rows % 32 == 0 and (rows * n_sp) % 256 == 0:
            return head_body(n_sp, inputs, w_query, w_key, *rest)
        return body(inputs, w_query, w_key, *rest)

    return jax.shard_map(
        whole_body,
        mesh=mesh,
        in_specs=(
            P("sp", None),
            P("dp", None),
            P("dp", None),
            P("dp", None),
            P(),
            P(),
            P("sp", "dp"),
        ),
        out_specs=(P("sp", "dp"), P("dp", None), P("dp", None), P("dp", None)),
        check_vma=False,
    )
```

```python
import functools

import jax
import jax.numpy as jnp
from jax import lax
from jax.experimental import pallas as pl
from jax.experimental.pallas import tpu as pltpu
from jax.sharding import PartitionSpec as P

HEAD_WIDTH = 64
GRID_W = 64


norm_eps = 1e-06
axial_base = 10000.0


def rotation_tables(offset, count):
    positions = offset + jnp.arange(count, dtype=jnp.int32)
    grid_rows = (positions // GRID_W).astype(jnp.float32)
    grid_cols = (positions % GRID_W).astype(jnp.float32)
    quarter = HEAD_WIDTH // 4
    freqs_axis = axial_base ** (-jnp.arange(quarter, dtype=jnp.float32) / quarter)
    angle_rows = grid_rows[:, None] * freqs_axis[None, :]
    angle_cols = grid_cols[:, None] * freqs_axis[None, :]
    cosine = jnp.concatenate(
        [jnp.cos(angle_rows), jnp.cos(angle_rows), jnp.cos(angle_cols), jnp.cos(angle_cols)], axis=1
    )
    sine = jnp.concatenate(
        [jnp.sin(angle_rows), jnp.sin(angle_rows), jnp.sin(angle_cols), jnp.sin(angle_cols)], axis=1
    )
    return (cosine, sine)


def quarter_turn(values):
    quarter = HEAD_WIDTH // 4
    return jnp.concatenate(
        [
            -values[..., quarter : 2 * quarter],
            values[..., :quarter],
            -values[..., 3 * quarter :],
            values[..., 2 * quarter : 3 * quarter],
        ],
        axis=-1,
    )


def quarter_back(values):
    quarter = HEAD_WIDTH // 4
    return jnp.concatenate(
        [
            values[..., quarter : 2 * quarter],
            -values[..., :quarter],
            values[..., 3 * quarter :],
            -values[..., 2 * quarter : 3 * quarter],
        ],
        axis=-1,
    )


def rotate(values, cosine, sine):
    return values * cosine + quarter_turn(values) * sine


def rotate_back(grads, cosine, sine):
    return grads * cosine + quarter_back(grads * sine)


def head_norm(raw):
    scale_inv = lax.rsqrt(jnp.mean(raw * raw, axis=-1, keepdims=True) + norm_eps)
    return (raw * scale_inv, scale_inv)


def head_norm_back(grads, normed, scale_inv, gain):
    scaled = grads * gain
    return scale_inv * (scaled - normed * jnp.mean(scaled * normed, axis=-1, keepdims=True))


def body(inputs, w_query, w_key, w_value, query_gain, key_gain, grad_out):
    tok_rows = inputs.shape[0]
    local_query = w_query.shape[0] // HEAD_WIDTH
    local_keys = w_key.shape[0] // HEAD_WIDTH
    group = local_query // local_keys
    key_width = local_keys * HEAD_WIDTH
    scale = HEAD_WIDTH ** (-0.5)
    contract = (((1,), (1,)), ((), ()))
    leading = (((0,), (0,)), ((), ()))
    offset = lax.axis_index("sp") * tok_rows
    cosine, sine = rotation_tables(offset, tok_rows)
    cos_wide = cosine[:, None, :]
    sin_wide = sine[:, None, :]
    q_raw = lax.dot_general(inputs, w_query, contract, preferred_element_type=jnp.float32).astype(
        jnp.bfloat16
    )
    w_pair = jnp.concatenate([w_key, w_value], axis=0)
    kv_raw = lax.dot_general(inputs, w_pair, contract, preferred_element_type=jnp.float32).astype(
        jnp.bfloat16
    )
    q_wide = (
        lax.optimization_barrier(q_raw)
        .astype(jnp.float32)
        .reshape(tok_rows, local_query, HEAD_WIDTH)
    )
    k_wide = (
        lax.optimization_barrier(kv_raw[:, :key_width])
        .astype(jnp.float32)
        .reshape(tok_rows, local_keys, HEAD_WIDTH)
    )
    q_normed, q_inv = head_norm(q_wide)
    k_normed, k_inv = head_norm(k_wide)
    q_rot = rotate(q_normed * query_gain, cos_wide, sin_wide).astype(jnp.bfloat16)
    k_rot = rotate(k_normed * key_gain, cos_wide, sin_wide).astype(jnp.bfloat16)
    kv_rot = jnp.concatenate([k_rot.reshape(tok_rows, key_width), kv_raw[:, key_width:]], axis=1)
    kv_every = lax.all_gather(kv_rot, "sp", axis=0, tiled=True)
    seq_rows = kv_every.shape[0]
    keys_every = kv_every[:, :key_width]
    values_every = kv_every[:, key_width:]
    grad_query = []
    log_totals = []
    deltas = []
    key_terms = [jnp.zeros((seq_rows, HEAD_WIDTH), jnp.float32) for slot in range(local_keys)]
    value_terms = [jnp.zeros((seq_rows, HEAD_WIDTH), jnp.float32) for slot in range(local_keys)]
    for member in range(local_query):
        kv_index = member // group
        query_head = q_rot[:, member, :]
        key_head = keys_every[:, kv_index * HEAD_WIDTH : (kv_index + 1) * HEAD_WIDTH]
        value_head = values_every[:, kv_index * HEAD_WIDTH : (kv_index + 1) * HEAD_WIDTH]
        grad_head = grad_out[:, member * HEAD_WIDTH : (member + 1) * HEAD_WIDTH]
        scores = (
            lax.dot_general(query_head, key_head, contract, preferred_element_type=jnp.float32)
            * scale
        )
        maxima = jnp.max(scores, axis=1, keepdims=True)
        log_total = maxima + jnp.log(jnp.sum(jnp.exp(scores - maxima), axis=1, keepdims=True))
        prob_exact = jnp.exp(scores - log_total)
        prob_half = prob_exact.astype(jnp.bfloat16)
        attn_rows = jnp.dot(prob_half, value_head, preferred_element_type=jnp.float32).astype(
            jnp.bfloat16
        )
        attn_wide = lax.optimization_barrier(attn_rows).astype(jnp.float32)
        delta_rows = jnp.sum(grad_head.astype(jnp.float32) * attn_wide, axis=1, keepdims=True)
        dprob = lax.dot_general(grad_head, value_head, contract, preferred_element_type=jnp.float32)
        dscore = (prob_exact * (dprob - delta_rows)).astype(jnp.bfloat16)
        grad_query.append(jnp.dot(dscore, key_head, preferred_element_type=jnp.float32) * scale)
        log_totals.append(log_total)
        deltas.append(delta_rows)
        value_terms[kv_index] = value_terms[kv_index] + lax.dot_general(
            prob_half, grad_head, leading, preferred_element_type=jnp.float32
        )
        key_terms[kv_index] = (
            key_terms[kv_index]
            + lax.dot_general(dscore, query_head, leading, preferred_element_type=jnp.float32)
            * scale
        )
    gradient_query_rotated = jnp.stack(grad_query, axis=1)
    partial_sums = jnp.concatenate(key_terms + value_terms, axis=1)
    own_grads = lax.psum_scatter(partial_sums, "sp", scatter_dimension=0, tiled=True)
    gradient_key_rotated = own_grads[:, :key_width].reshape(tok_rows, local_keys, HEAD_WIDTH)
    grad_q = head_norm_back(
        rotate_back(gradient_query_rotated, cos_wide, sin_wide), q_normed, q_inv, query_gain
    )
    grad_q = grad_q.reshape(tok_rows, local_query * HEAD_WIDTH).astype(jnp.bfloat16)
    grad_k = head_norm_back(
        rotate_back(gradient_key_rotated, cos_wide, sin_wide), k_normed, k_inv, key_gain
    )
    grad_kv = jnp.concatenate(
        [
            grad_k.reshape(tok_rows, key_width).astype(jnp.bfloat16),
            own_grads[:, key_width:].astype(jnp.bfloat16),
        ],
        axis=1,
    )
    head_part = jnp.dot(grad_q, w_query, preferred_element_type=jnp.float32)
    head_part = head_part + jnp.dot(grad_kv, w_pair, preferred_element_type=jnp.float32)
    d_inputs = lax.psum_scatter(
        head_part.astype(jnp.bfloat16), "dp", scatter_dimension=1, tiled=True
    )
    grad_wq = lax.dot_general(grad_q, inputs, leading, preferred_element_type=jnp.float32)
    grad_wkv = lax.dot_general(grad_kv, inputs, leading, preferred_element_type=jnp.float32)
    grad_wq, grad_wkv = lax.psum((grad_wq, grad_wkv), "sp")
    return (d_inputs, grad_wq, grad_wkv[:key_width], grad_wkv[key_width:])


MESH = pl.DeviceIdType.MESH
VMEM_LIMIT = 60 * 1024 * 1024


def turn(values):
    quarter = HEAD_WIDTH // 4
    return jnp.concatenate(
        [
            -values[quarter : 2 * quarter],
            values[:quarter],
            -values[3 * quarter :],
            values[2 * quarter : 3 * quarter],
        ],
        axis=0,
    )


def turn_back(values):
    return -turn(values)


def norm_cols(raw):
    inv = lax.rsqrt(jnp.mean(raw * raw, axis=0, keepdims=True) + norm_eps)
    return raw * inv, inv


def norm_cols_back(grads, normed, inv, gain):
    scaled = grads * gain
    return inv * (scaled - normed * jnp.mean(scaled * normed, axis=0, keepdims=True))


def other_of_pair(index):
    return index + 1 - 2 * lax.rem(index, 2)


def gather_kernel(n, x_ref, g_ref, xall, gall, xsend, xrecv, gsend, grecv, fsend, frecv, own):
    me = lax.axis_index("sp")
    core = lax.rem(lax.axis_index("dp"), 2)
    twin = other_of_pair(lax.axis_index("dp"))
    half = x_ref.shape[0] // 2
    mine = pl.ds(pl.multiple_of(core * half, 16), half)
    theirs = pl.ds(pl.multiple_of((1 - core) * half, 16), half)
    barrier = pltpu.get_barrier_semaphore()
    for off in range(1, n):
        pl.semaphore_signal(
            barrier, inc=1, device_id={"sp": lax.rem(me + off, n)}, device_id_type=MESH
        )
    pl.semaphore_signal(barrier, inc=1, device_id={"dp": twin}, device_id_type=MESH)
    pl.semaphore_wait(barrier, n)
    sends = []
    for off in range(1, n):
        peer = lax.rem(me + off, n)
        sends.append(
            pltpu.make_async_remote_copy(
                src_ref=g_ref.at[peer],
                dst_ref=gall.at[me],
                send_sem=gsend.at[off - 1],
                recv_sem=grecv.at[off - 1],
                device_id={"sp": peer},
                device_id_type=MESH,
            )
        )
    mate = other_of_pair(me)

    def move(source, slot, device, part=mine, pair=(xsend, xrecv), first=False):
        return pltpu.make_async_remote_copy(
            src_ref=x_ref.at[mine] if first else xall.at[source, mine],
            dst_ref=xall.at[source, part],
            send_sem=pair[0].at[slot],
            recv_sem=pair[1].at[slot],
            device_id=device,
            device_id_type=MESH,
        )

    for off in range(2, n, 2):
        sends.append(move(me, off - 1, {"sp": lax.rem(me + off, n)}, first=True))
    sends.append(move(me, 0, {"sp": mate}, first=True))
    for copy in sends:
        copy.start()
    own_x = pltpu.make_async_copy(x_ref, xall.at[me], own.at[0])
    own_g = pltpu.make_async_copy(g_ref.at[me], gall.at[me], own.at[1])
    own_x.start()
    own_g.start()
    forwards = (fsend, frecv)
    for slot in range(0, n, 2):
        source = lax.rem(mate + n - slot, n)
        move(source, slot, {"sp": mate}).wait_recv()
        move(source, slot, {"dp": twin}, pair=forwards).start()
        if slot + 2 < n:
            source = lax.rem(me + n - slot - 2, n)
            move(source, slot + 1, {"sp": source}).wait_recv()
            relay = move(source, slot + 2, {"sp": mate})
            relay.start()
            sends.append(relay)
            move(source, slot + 1, {"dp": twin}, pair=forwards).start()
    for off in range(1, n):
        source = lax.rem(me + n - off, n)
        pltpu.make_async_remote_copy(
            src_ref=g_ref.at[source],
            dst_ref=gall.at[source],
            send_sem=gsend.at[off - 1],
            recv_sem=grecv.at[off - 1],
            device_id={"sp": source},
            device_id_type=MESH,
        ).wait_recv()
    for slot in range(n - 1):
        base = me if slot % 2 else mate
        source = lax.rem(base + n - (slot + slot % 2), n)
        move(source, slot, {"dp": twin}, part=theirs, pair=forwards).wait()
    for copy in sends:
        copy.wait_send()
    own_x.wait()
    own_g.wait()


def gather_call(n, x, g_parts):
    rows, width = x.shape
    dma = pltpu.SemaphoreType.DMA
    return pl.pallas_call(
        functools.partial(gather_kernel, n),
        out_shape=(
            jax.ShapeDtypeStruct((n, rows, width), x.dtype),
            jax.ShapeDtypeStruct(g_parts.shape, g_parts.dtype),
        ),
        in_specs=[pl.BlockSpec(memory_space=pltpu.VMEM)] * 2,
        out_specs=[pl.BlockSpec(memory_space=pl.ANY)] * 2,
        scratch_shapes=[dma((n - 1,))] * 6 + [dma((2,))],
        compiler_params=pltpu.CompilerParams(
            collective_id=0, has_side_effects=True, vmem_limit_bytes=VMEM_LIMIT
        ),
        name="gather_tokens",
    )(x, g_parts)


def head_kernel(
    tile, x_ref, w_ref, g_ref, cos_ref, sin_ref, qg_ref, kg_ref,
    gq_ref, mine_ref, theirs_ref, kn_ref, rk_ref,
    q_t, q_n, q_r, k_t, v_t, k_s, v_s, g_t, k_n, k_r, dk, dv,
):
    seq = x_ref.shape[0]
    width = HEAD_WIDTH
    scale = width ** (-0.5)
    contract = (((1,), (1,)), ((), ()))

    @pl.loop(0, seq // tile)
    def _(step):
        cols = pl.ds(pl.multiple_of(step * tile, tile), tile)
        raw = lax.dot_general(
            w_ref[...], x_ref[cols, :], contract, preferred_element_type=jnp.float32
        ).astype(jnp.bfloat16)
        wide = raw.astype(jnp.float32)
        cosine = cos_ref[:, cols]
        sine = sin_ref[:, cols]
        normed, inv = norm_cols(wide[:width])
        gained = normed * qg_ref[...]
        rot = (gained * cosine + turn(gained) * sine).astype(jnp.bfloat16)
        q_t[:, cols] = (rot.astype(jnp.float32) * scale).astype(jnp.bfloat16)
        q_n[:, cols] = normed
        q_r[:, cols] = inv
        normed, inv = norm_cols(wide[width : 2 * width])
        gained = normed * kg_ref[...]
        rot = (gained * cosine + turn(gained) * sine).astype(jnp.bfloat16)
        k_t[:, cols] = rot
        k_s[cols, :] = rot.astype(jnp.float32).T.astype(jnp.bfloat16)
        k_n[:, cols] = normed
        k_r[:, cols] = inv
        v_t[:, cols] = raw[2 * width :]
        v_s[cols, :] = wide[2 * width :].T.astype(jnp.bfloat16)
        g_t[:, cols] = g_ref[cols, :].astype(jnp.float32).T.astype(jnp.bfloat16)

    dk[...] = jnp.zeros_like(dk)
    dv[...] = jnp.zeros_like(dv)

    @pl.loop(0, seq // tile)
    def _(step):
        cols = pl.ds(pl.multiple_of(step * tile, tile), tile)
        query = q_t[:, cols]
        grad = g_t[:, cols]
        scores = jnp.dot(k_s[...], query, preferred_element_type=jnp.float32)
        maxima = jnp.max(scores, axis=0, keepdims=True)
        powers = jnp.exp(scores - maxima)
        prob = powers * (1.0 / jnp.sum(powers, axis=0, keepdims=True))
        prob_half = prob.astype(jnp.bfloat16)
        attn = jnp.dot(v_t[...], prob_half, preferred_element_type=jnp.float32).astype(jnp.bfloat16)
        delta = jnp.sum(grad.astype(jnp.float32) * attn.astype(jnp.float32), axis=0, keepdims=True)
        dv[...] += lax.dot_general(grad, prob_half, contract, preferred_element_type=jnp.float32)
        dprob = jnp.dot(v_s[...], grad, preferred_element_type=jnp.float32)
        dscore = (prob * (dprob - delta)).astype(jnp.bfloat16)
        dk[...] += lax.dot_general(query, dscore, contract, preferred_element_type=jnp.float32)
        dq = jnp.dot(k_t[...], dscore, preferred_element_type=jnp.float32) * scale
        back = dq * cos_ref[:, cols] + turn_back(dq * sin_ref[:, cols])
        gq_ref[:, cols] = norm_cols_back(back, q_n[:, cols], q_r[:, cols], qg_ref[...]).astype(
            jnp.bfloat16
        )

    parity = lax.rem(lax.axis_index("sp"), 2)
    half = seq // 2
    own = pl.ds(pl.multiple_of(parity * half, 128), half)
    other = pl.ds(pl.multiple_of((1 - parity) * half, 128), half)
    mine_ref[0] = dk[:, own]
    mine_ref[1] = dv[:, own]
    theirs_ref[0] = dk[:, other].astype(jnp.bfloat16)
    theirs_ref[1] = dv[:, other].astype(jnp.bfloat16)
    kn_ref[...] = k_n[:, own]
    rk_ref[...] = k_r[:, own]


def head_call(x_all, w_head, g_head, cosine, sine, q_gain, k_gain):
    seq = x_all.shape[0]
    width = HEAD_WIDTH
    half = seq // 2
    f32, bf16 = jnp.float32, jnp.bfloat16
    tile = 256
    return pl.pallas_call(
        functools.partial(head_kernel, tile),
        out_shape=(
            jax.ShapeDtypeStruct((width, seq), bf16),
            jax.ShapeDtypeStruct((2, width, half), f32),
            jax.ShapeDtypeStruct((2, width, half), bf16),
            jax.ShapeDtypeStruct((width, half), f32),
            jax.ShapeDtypeStruct((1, half), f32),
        ),
        in_specs=[pl.BlockSpec(memory_space=pltpu.VMEM)] * 7,
        out_specs=[pl.BlockSpec(memory_space=pltpu.VMEM)] * 5,
        scratch_shapes=[
            pltpu.VMEM((width, seq), bf16),
            pltpu.VMEM((width, seq), f32),
            pltpu.VMEM((1, seq), f32),
            pltpu.VMEM((width, seq), bf16),
            pltpu.VMEM((width, seq), bf16),
            pltpu.VMEM((seq, width), bf16),
            pltpu.VMEM((seq, width), bf16),
            pltpu.VMEM((width, seq), bf16),
            pltpu.VMEM((width, seq), f32),
            pltpu.VMEM((1, seq), f32),
            pltpu.VMEM((width, seq), f32),
            pltpu.VMEM((width, seq), f32),
        ],
        compiler_params=pltpu.CompilerParams(vmem_limit_bytes=VMEM_LIMIT),
        name="one_head",
    )(x_all, w_head, g_head, cosine, sine, q_gain, k_gain)


def spread_kernel(
    n, gq_ref, mine_ref, theirs_ref, kn_ref, rk_ref, cos_ref, sin_ref, kg_ref,
    gq_all, gkv_all, landed, gkv, qsend, qrecv, ksend, krecv, own,
):
    me = lax.axis_index("sp")
    mate = other_of_pair(me)
    half = mine_ref.shape[2]

    def place(index):
        columns = pl.ds(pl.multiple_of(lax.rem(index, 2) * half, 128), half)
        return gkv_all.at[:, index // 2, :, columns]

    barrier = pltpu.get_barrier_semaphore()
    for off in range(1, n):
        pl.semaphore_signal(
            barrier, inc=1, device_id={"sp": lax.rem(me + off, n)}, device_id_type=MESH
        )
    pl.semaphore_wait(barrier, n - 1)
    swap = pltpu.make_async_remote_copy(
        src_ref=theirs_ref,
        dst_ref=landed,
        send_sem=own.at[0],
        recv_sem=own.at[1],
        device_id={"sp": mate},
        device_id_type=MESH,
    )
    swap.start()

    def move_q(source, slot, device, first=False):
        return pltpu.make_async_remote_copy(
            src_ref=gq_ref if first else gq_all.at[source],
            dst_ref=gq_all.at[source],
            send_sem=qsend.at[slot],
            recv_sem=qrecv.at[slot],
            device_id={"sp": device},
            device_id_type=MESH,
        )

    def move_k(source, slot, device, first=False):
        return pltpu.make_async_remote_copy(
            src_ref=gkv if first else place(source),
            dst_ref=place(source),
            send_sem=ksend.at[slot],
            recv_sem=krecv.at[slot],
            device_id={"sp": device},
            device_id_type=MESH,
        )

    def start_all(move):
        copies = [move(me, off - 1, lax.rem(me + off, n), True) for off in range(2, n, 2)]
        copies.append(move(me, 0, mate, True))
        for copy in copies:
            copy.start()
        return copies

    sends = start_all(move_q)
    own_q = pltpu.make_async_copy(gq_ref, gq_all.at[me], own.at[2])
    own_q.start()
    swap.wait()
    dkey = mine_ref[0] + landed[0].astype(jnp.float32)
    back = dkey * cos_ref[...] + turn_back(dkey * sin_ref[...])
    gkv[0] = norm_cols_back(back, kn_ref[...], rk_ref[...], kg_ref[...]).astype(jnp.bfloat16)
    gkv[1] = (mine_ref[1] + landed[1].astype(jnp.float32)).astype(jnp.bfloat16)
    sends += start_all(move_k)
    own_k = pltpu.make_async_copy(gkv, place(me), own.at[3])
    own_k.start()
    for move in (move_q, move_k):
        for slot in range(0, n, 2):
            if slot + 2 < n:
                source = lax.rem(me + n - slot - 2, n)
                move(source, slot + 1, source).wait_recv()
                relay = move(source, slot + 2, mate)
                relay.start()
                sends.append(relay)
    for move in (move_q, move_k):
        for slot in range(0, n, 2):
            move(lax.rem(mate + n - slot, n), slot, mate).wait_recv()
    for copy in sends:
        copy.wait_send()
    own_q.wait()
    own_k.wait()


def spread_call(n, gq, mine, theirs, k_normed, k_inv, cosine, sine, k_gain):
    width, seq = gq.shape
    half = seq // 2
    bf16 = jnp.bfloat16
    dma = pltpu.SemaphoreType.DMA
    return pl.pallas_call(
        functools.partial(spread_kernel, n),
        out_shape=(
            jax.ShapeDtypeStruct((n, width, seq), bf16),
            jax.ShapeDtypeStruct((2, n // 2, width, seq), bf16),
        ),
        in_specs=[pl.BlockSpec(memory_space=pltpu.VMEM)] * 8,
        out_specs=[pl.BlockSpec(memory_space=pl.ANY)] * 2,
        scratch_shapes=[
            pltpu.VMEM((2, width, half), bf16),
            pltpu.VMEM((2, width, half), bf16),
            dma((n - 1,)),
            dma((n - 1,)),
            dma((n - 1,)),
            dma((n - 1,)),
            dma((4,)),
        ],
        compiler_params=pltpu.CompilerParams(
            collective_id=1, has_side_effects=True, vmem_limit_bytes=VMEM_LIMIT
        ),
        name="spread_grads",
    )(gq, mine, theirs, k_normed, k_inv, cosine, sine, k_gain)


def axial_columns(seq):
    quarter = HEAD_WIDTH // 4
    freqs = axial_base ** (-jnp.arange(quarter, dtype=jnp.float32) / quarter)
    grid_rows = -(-seq // GRID_W)
    by_row = freqs[:, None] * jnp.arange(grid_rows, dtype=jnp.float32)[None, :]
    by_col = freqs[:, None] * jnp.arange(GRID_W, dtype=jnp.float32)[None, :]

    def table(function):
        rows = jnp.repeat(function(by_row), GRID_W, axis=1)[:, :seq]
        cols = jnp.tile(function(by_col), (1, grid_rows))[:, :seq]
        return jnp.concatenate([rows, rows, cols, cols], axis=0)

    return table(jnp.cos), table(jnp.sin)


def head_body(n, inputs, w_query, w_key, w_value, query_gain, key_gain, grad_out):
    rows = inputs.shape[0]
    seq = rows * n
    width = HEAD_WIDTH
    me = lax.axis_index("sp")
    g_parts = grad_out.reshape(rows, n, width).transpose(1, 0, 2)
    cosine, sine = axial_columns(seq)
    w_head = jnp.concatenate(
        [
            lax.dynamic_slice_in_dim(w_query, me * width, width, 0),
            lax.dynamic_slice_in_dim(w_key, (me // 2) * width, width, 0),
            lax.dynamic_slice_in_dim(w_value, (me // 2) * width, width, 0),
        ],
        axis=0,
    )
    q_gain = query_gain[:, None]
    k_gain = key_gain[:, None]
    x_all, g_all = gather_call(n, inputs, g_parts)
    x_all = x_all.reshape(seq, inputs.shape[1])
    gq, mine, theirs, k_normed, k_inv = head_call(
        x_all, w_head, g_all.reshape(seq, width), cosine, sine, q_gain, k_gain
    )
    half = seq // 2
    start = (me % 2) * half
    gq_all, gkv_all = spread_call(
        n, gq, mine, theirs, k_normed, k_inv,
        lax.dynamic_slice_in_dim(cosine, start, half, 1),
        lax.dynamic_slice_in_dim(sine, start, half, 1),
        k_gain,
    )
    grads = [
        gq_all.reshape(n * width, seq),
        gkv_all[0].reshape(n // 2 * width, seq),
        gkv_all[1].reshape(n // 2 * width, seq),
    ]
    head_part = 0.0
    for grad, weight in zip(grads, (w_query, w_key, w_value)):
        own = lax.dynamic_slice_in_dim(grad, me * rows, rows, 1)
        head_part = head_part + lax.dot_general(
            own, weight, (((0,), (0,)), ((), ())), preferred_element_type=jnp.float32
        )
    d_inputs = lax.psum_scatter(
        head_part.astype(jnp.bfloat16), "dp", scatter_dimension=1, tiled=True
    )
    outs = [jnp.dot(grad, x_all, preferred_element_type=jnp.float32) for grad in grads]
    return (d_inputs, *outs)


def solution(mesh):
    n_sp = mesh.shape["sp"]
    n_dp = mesh.shape["dp"]

    def whole_body(inputs, w_query, w_key, *rest):
        heads = w_query.shape[0] // HEAD_WIDTH
        rows = inputs.shape[0]
        fits = heads == n_sp and w_query.shape[0] == 2 * w_key.shape[0] and n_dp % 2 == 0
        if fits and n_sp % 2 == 0 and rows % 32 == 0 and (rows * n_sp) % 256 == 0:
            return head_body(n_sp, inputs, w_query, w_key, *rest)
        return body(inputs, w_query, w_key, *rest)

    return jax.shard_map(
        whole_body,
        mesh=mesh,
        in_specs=(
            P("sp", None),
            P("dp", None),
            P("dp", None),
            P("dp", None),
            P(),
            P(),
            P("sp", "dp"),
        ),
        out_specs=(P("sp", "dp"), P("dp", None), P("dp", None), P("dp", None)),
        check_vma=False,
    )
```
